32 devices in a mesh: dp: 4 (over y, x), kv: 4 (over z), tp: 2 (over core).
Axes of the slice: x: 2, y: 2, z: 4, core: 2. Of those that a mesh axis runs over, the one named last changes fastest.
Arguments:
- tokens: bfloat16 [8192, 2048], P(('dp', 'kv')), parts along dimension 0, may hold values from -60 to 60, as said below
- chosen: int32 [128, 16], P(('dp', 'kv')), parts along dimension 0, may hold values from -1 to 31, as said below
- query_weight: bfloat16 [2048, 1024], P('kv', 'tp'), may hold values from -0.125 to 0.125
- key_matrix: bfloat16 [2048, 128], P('kv', 'tp'), may hold values from -0.125 to 0.125
- value_matrix: bfloat16 [2048, 128], P('kv', 'tp'), may hold values from -0.125 to 0.125
- out_weight: bfloat16 [1024, 2048], P('tp', 'kv'), may hold values from -0.1875 to 0.1875
- out_gain: float32 [2048], replicated, may hold values from 0.1 to 1.9
Outputs:
- mixed_out: bfloat16 [8192, 2048], P(('dp', 'kv', 'tp')), parts along dimension 0
The draws below stay inside these ranges and needn't reach their ends.
There are 4 independent parts, one for each index of `dp`. The reference program is written for one: setup_inputs(seed, part) draws one part's arguments, and reference() takes and returns one part's arrays. A program takes and returns all parts, laid end to end along the dimension named above; an argument that names none is the same for every part. Nothing has to cross between parts.
Inputs may be any that keep to these rules, and one draw needn't show every extreme that they name: tokens are of order one apart from few rows. chosen[g, 0] = g; every other entry of row g is -1 or a block below g, and the entries of a row other than -1 are distinct; the blocks that the rows of one device name on any single other device are at most 2 different ones, and this is reached.
All inputs are finite; a program needn't handle non-finite values.
Results may differ from the reference program's by a relative error of at most 0.012.
The reference program's roundings to bfloat16 on the way count: a program that leaves them out, or rounds other values in their place, can miss the bound.
Values may be sent and summed in bfloat16 or wider, within the bound.
No kernel may reach another device: no remote copies, remote signals or barrier semaphores. Data moves between devices by JAX's collectives and lax.ppermute only.
A program may use at most 64 MiB of HBM per device.

```python
import jax
import jax.numpy as jnp
from jax import lax

MODEL_WIDTH = 2048
QUERY_HEADS = 16
KEY_VALUE_HEADS = 2
HEAD_WIDTH = 64
BLOCK_LENGTH = 64
SEL = 16
CAP = 2
SEQ = 2048
BLOCKS_DEV = 8
SEQUENCE_BLOCKS = 32
N_KV = 4


def draw_tokens(key, part):
    base = jax.random.normal(key, (SEQ, MODEL_WIDTH), jnp.float32)
    return jnp.clip(base, -60.0, 60.0).astype(jnp.bfloat16)


def draw_chosen(key, part):
    owners = N_KV
    per_dev = BLOCKS_DEV
    parts_keys = jax.random.split(key, 3)
    requester = jnp.arange(owners, dtype=jnp.int32)[:, None]
    holder = jnp.arange(owners, dtype=jnp.int32)[None, :]
    roll = jax.random.randint(parts_keys[0], (owners, owners), 0, 8)
    favored = (holder == 0) | (holder == requester - 1) | (holder == requester - owners // 2)
    counts = jnp.where(favored | (roll < 2), CAP, jnp.where(roll < 4, 1, 0))
    counts = jnp.where(holder < requester, counts, 0)
    order = jax.random.randint(parts_keys[1], (owners, owners, per_dev), 0, 1 << 20) * 1024 + jnp.arange(per_dev, dtype=jnp.int32)
    _, first = lax.top_k(order, min(CAP, per_dev))
    first = jnp.concatenate([first, jnp.zeros((owners, owners, CAP - first.shape[-1]), jnp.int32)], axis=-1)
    slot_index = jnp.arange(CAP, dtype=jnp.int32)
    counts = jnp.minimum(counts, per_dev)
    remote_ids = (holder[:, :, None] * per_dev + first).reshape(owners, owners * CAP)
    remote_live = (slot_index[None, None, :] < counts[:, :, None]).reshape(owners, owners * CAP)
    remote_tier = jnp.broadcast_to(jnp.where(favored, 2, 1)[:, :, None], (owners, owners, CAP)).reshape(owners, owners * CAP)
    local_pos = jnp.arange(per_dev, dtype=jnp.int32)
    local_ids = jnp.broadcast_to((requester * per_dev + local_pos[None, :])[:, None, :], (owners, per_dev, per_dev))
    local_live = jnp.broadcast_to((local_pos[None, :] < local_pos[:, None])[None], (owners, per_dev, per_dev))
    pad_ids = jnp.zeros((owners, per_dev, SEL), jnp.int32)
    pad_live = jnp.zeros((owners, per_dev, SEL), bool)
    cand_ids = jnp.concatenate([jnp.broadcast_to(remote_ids[:, None, :], (owners, per_dev, owners * CAP)), local_ids, pad_ids], axis=-1)
    cand_live = jnp.concatenate([jnp.broadcast_to(remote_live[:, None, :], (owners, per_dev, owners * CAP)), local_live, pad_live], axis=-1)
    cand_tier = jnp.concatenate([jnp.broadcast_to(remote_tier[:, None, :], (owners, per_dev, owners * CAP)), jnp.ones((owners, per_dev, per_dev), jnp.int32), jnp.zeros((owners, per_dev, SEL), jnp.int32)], axis=-1)
    cand_width = owners * CAP + per_dev + SEL
    cand_index = jnp.arange(cand_width, dtype=jnp.int32)[None, None, :]
    noise = jax.random.randint(parts_keys[2], (owners, per_dev, cand_width), 0, 1 << 17)
    score = jnp.where(cand_live, cand_tier * (1 << 28) + noise * 2048 + cand_index, cand_index)
    _, position = lax.top_k(score, SEL - 1)
    taken = jnp.take_along_axis(cand_ids, position, axis=-1)
    live = jnp.take_along_axis(cand_live, position, axis=-1)
    others = jnp.where(live, taken, -1)
    own_ids = (requester * per_dev + local_pos[None, :])[:, :, None]
    return jnp.concatenate([own_ids, others], axis=-1).reshape(owners * per_dev, SEL).astype(jnp.int32)


def block_scale(key, dims, cuts, smallest, high):
    def one(dim, parts):
        heights = jax.random.uniform(jax.random.fold_in(jax.random.fold_in(key, 6), dim), (parts,), jnp.float32, smallest / len(cuts), high / len(cuts))
        return jnp.repeat(jnp.exp(heights), dims[dim] // parts).reshape((-1,) + (1,) * (len(dims) - dim - 1))

    gain = one(*cuts[0])
    for cut in cuts[1:]:
        gain = gain * one(*cut)
    return gain


def centred(stream_key, shape, spread, reach, shards=(), kind=jnp.bfloat16):
    gain = block_scale(stream_key, shape, shards, -0.22, 0.18) if shards else 1.0
    array = jax.random.normal(stream_key, shape, jnp.float32) * spread * gain
    return jnp.minimum(jnp.maximum(array, -reach), reach).astype(kind)


def setup_inputs(seed: int = 0, part: int = 0) -> dict:
    splits = jax.random.split(jax.random.key(seed), 8)
    own_keys = jax.random.split(jax.random.fold_in(splits[7], part), 8)
    return {
        "tokens": draw_tokens(jax.random.fold_in(jax.random.fold_in(splits[7], part), 71), part),
        "chosen": draw_chosen(jax.random.fold_in(jax.random.fold_in(splits[7], part), 71), part),
        "query_weight": centred(splits[2], (MODEL_WIDTH, QUERY_HEADS * HEAD_WIDTH), MODEL_WIDTH ** -0.5, 0.125, ((0, 4), (1, 2))),
        "key_matrix": centred(splits[3], (MODEL_WIDTH, KEY_VALUE_HEADS * HEAD_WIDTH), MODEL_WIDTH ** -0.5, 0.125, ((0, 4), (1, 2))),
        "value_matrix": centred(splits[4], (MODEL_WIDTH, KEY_VALUE_HEADS * HEAD_WIDTH), MODEL_WIDTH ** -0.5, 0.125, ((0, 4), (1, 2))),
        "out_weight": centred(splits[5], (QUERY_HEADS * HEAD_WIDTH, MODEL_WIDTH), (QUERY_HEADS * HEAD_WIDTH) ** -0.5, 0.1875, ((0, 2), (1, 4))),
        "out_gain": jnp.clip(1.0 + 0.18 * jax.random.normal(splits[6], (MODEL_WIDTH,), jnp.float32), 0.1, 1.9),
    }


def reference(tokens, chosen, query_weight, key_matrix, value_matrix, out_weight, out_gain):
    head_groups = QUERY_HEADS // KEY_VALUE_HEADS
    query_rows = jnp.dot(tokens, query_weight, preferred_element_type=jnp.float32).astype(jnp.bfloat16)
    key_rows = jnp.dot(tokens, key_matrix, preferred_element_type=jnp.float32).astype(jnp.bfloat16)
    value_rows = jnp.dot(tokens, value_matrix, preferred_element_type=jnp.float32).astype(jnp.bfloat16)
    blocked_queries = query_rows.reshape(SEQUENCE_BLOCKS, BLOCK_LENGTH, KEY_VALUE_HEADS, head_groups, HEAD_WIDTH)
    blocked_keys = key_rows.reshape(SEQUENCE_BLOCKS, BLOCK_LENGTH, KEY_VALUE_HEADS, HEAD_WIDTH)
    blocked_values = value_rows.reshape(SEQUENCE_BLOCKS, BLOCK_LENGTH, KEY_VALUE_HEADS, HEAD_WIDTH)
    offsets = jnp.arange(BLOCK_LENGTH, dtype=jnp.int32)
    score_scale = HEAD_WIDTH ** (-0.5)

    def one_block(inputs):
        block, row_ids, index = inputs
        safe_ids = jnp.maximum(row_ids, 0).astype(jnp.int32)
        picked_keys = blocked_keys[safe_ids].astype(jnp.float32)
        picked_values = blocked_values[safe_ids].astype(jnp.float32)
        query_pos = index * BLOCK_LENGTH + offsets
        key_pos = safe_ids[:, None] * BLOCK_LENGTH + offsets[None, :]
        visible = (row_ids >= 0)[None, :, None] & (key_pos[None, :, :] <= query_pos[:, None, None])
        scores = jnp.einsum('qhgd,skhd->hgqsk', block.astype(jnp.float32), picked_keys) * score_scale
        scores = jnp.where(visible[None, None], scores, -1e+30)
        row_max = lax.optimization_barrier(jnp.max(scores, axis=(3, 4), keepdims=True))
        expon = jnp.exp(scores - row_max)
        row_sum = lax.optimization_barrier(jnp.sum(expon, axis=(3, 4), keepdims=True))
        weights_bf = (expon / row_sum).astype(jnp.bfloat16)
        result = jnp.einsum('hgqsk,skhd->qhgd', weights_bf.astype(jnp.float32), picked_values)
        return result.astype(jnp.bfloat16)
    attended = lax.map(one_block, (blocked_queries, chosen, jnp.arange(SEQUENCE_BLOCKS, dtype=jnp.int32)))
    attended = attended.reshape(SEQ, QUERY_HEADS * HEAD_WIDTH)
    mixed = jnp.dot(attended, out_weight, preferred_element_type=jnp.float32)
    normed = mixed * lax.rsqrt(lax.optimization_barrier(jnp.mean(mixed * mixed, axis=-1, keepdims=True)) + 1e-06) * out_gain.astype(jnp.float32)
    return normed.astype(jnp.bfloat16)
```

```python
import functools

import jax
import jax.numpy as jnp
from jax import lax
from jax.experimental import pallas as pl
from jax.experimental.pallas import tpu as pltpu
from jax.sharding import PartitionSpec as P

HEAD_WIDTH = 64
BLOCK_LENGTH = 64
ALIGN = 16
LOG2E = 1.4426950408889634
BF16 = jnp.bfloat16
F32 = jnp.float32


def shift(x, axis, by, count):
    return lax.ppermute(x, axis, [(i, (i + by) % count) for i in range(count)])


def swap(x, axis, bit, count):
    return lax.ppermute(x, axis, [(i, i ^ bit) for i in range(count)])


def spread(w, kv_count, dp_count):
    rows = w.shape[0] // dp_count
    half = rows // 2
    dp = lax.axis_index("dp")
    piece = lax.dynamic_slice_in_dim(w, dp * rows, rows, axis=0)
    got = [shift(piece, "kv", s, kv_count) for s in range(1, kv_count)]
    mine = jnp.concatenate([g[:half] for g in got] + [g[half:] for g in got], axis=0)
    cut = half * (kv_count - 1)
    across = swap(mine, "dp", 1, dp_count)
    along = swap(mine, "dp", 2, dp_count)
    far_top = swap(across[:cut], "dp", 2, dp_count)
    far_low = swap(along[cut:], "dp", 1, dp_count)
    return [w, mine, across, along, far_top, far_low]


def place(refs, dest, kv, dp, kv_count, dp_count):
    if len(refs) == 1:
        dest[...] = refs[0][...].reshape(dest.shape)
        return
    own, mine, across, along, far_top, far_low = refs
    dest[pl.ds(kv, 1)] = own[...][None]
    rows = own.shape[0] // dp_count
    half = rows // 2
    cut = half * (kv_count - 1)
    for s in range(1, kv_count):
        source = lax.rem(kv - s + kv_count, kv_count)
        at = half * (s - 1)
        for h in range(2):
            for bits, ref, base in (
                (0, mine, h * cut),
                (1, across, h * cut),
                (2, along, h * cut),
                (3, (far_top, far_low)[h], 0),
            ):
                first = pl.multiple_of((dp ^ bits) * rows + h * half, half)
                dest[pl.ds(source, 1), pl.ds(first, half)] = ref[pl.ds(base + at, half)][None]


def attend_kernel(where_ref, chosen_ref, tok_ref, *refs, n_weights, n_rows, kv_count, dp_count, heads):
    w_refs = refs[:n_weights]
    row_refs = refs[n_weights:n_weights + n_rows]
    out_ref, w_full, kv_full, q_full, picked = refs[n_weights + n_rows:]
    kv = where_ref[0]
    dp = where_ref[1]
    place(w_refs, w_full, kv, dp, kv_count, dp_count)
    if n_rows == 1:
        kv_full[...] = row_refs[0][...]
    else:
        count = row_refs[0].shape[0]
        for s, ref in enumerate(row_refs):
            source = lax.rem(kv - s + kv_count, kv_count)
            kv_full[pl.ds(pl.multiple_of(source * count, count), count)] = ref[...]
    whole = w_full[...].reshape(-1, w_full.shape[-1])
    queries = jnp.dot(tok_ref[...], whole, preferred_element_type=F32).astype(BF16)
    q_full[...] = queries
    blocks, sel = chosen_ref.shape
    wide = heads * BLOCK_LENGTH
    key_at = lax.broadcasted_iota(jnp.int32, (BLOCK_LENGTH, wide), 0)
    query_at = lax.rem(lax.broadcasted_iota(jnp.int32, (BLOCK_LENGTH, wide), 1), BLOCK_LENGTH)
    causal = key_at <= query_at
    factor = HEAD_WIDTH ** (-0.5) * LOG2E

    def one_block(g, carry):
        at = pl.multiple_of(g * BLOCK_LENGTH, BLOCK_LENGTH)
        qg = q_full[pl.ds(at, BLOCK_LENGTH)]
        stacked = jnp.concatenate(
            [qg[:, h * HEAD_WIDTH:(h + 1) * HEAD_WIDTH] for h in range(heads)], axis=0
        )
        stacked = jnp.concatenate([stacked, jnp.zeros_like(stacked)], axis=1)
        bias = []
        for s in range(sel):
            name = chosen_ref[g, s]
            first = pl.multiple_of(jnp.maximum(name, 0) * BLOCK_LENGTH, BLOCK_LENGTH)
            picked[s * BLOCK_LENGTH:(s + 1) * BLOCK_LENGTH] = kv_full[pl.ds(first, BLOCK_LENGTH)]
            bias.append(jnp.where(name < 0, F32(-1e30), F32(0)))
        pairs = picked[...]
        scores = lax.dot_general(
            pairs, stacked, (((1,), (1,)), ((), ())), preferred_element_type=F32
        )
        parts = []
        top = None
        for s in range(sel):
            part = scores[s * BLOCK_LENGTH:(s + 1) * BLOCK_LENGTH]
            part = jnp.where(causal, part, -1e30) if s == 0 else part + bias[s]
            parts.append(part)
            peak = jnp.max(part, axis=0, keepdims=True)
            top = peak if top is None else jnp.maximum(top, peak)
        total = None
        probs = []
        for part in parts:
            e = jnp.exp2((part - top) * factor)
            add = jnp.sum(e, axis=0, keepdims=True)
            total = add if total is None else total + add
            probs.append(e.astype(BF16))
        prob = jnp.concatenate(probs, axis=0)
        mixed = lax.dot_general(
            pairs, prob, (((0,), (0,)), ((), ())), preferred_element_type=F32
        )
        outcome = (mixed[HEAD_WIDTH:] / total).T
        out_ref[pl.ds(at, BLOCK_LENGTH)] = jnp.concatenate(
            [outcome[h * BLOCK_LENGTH:(h + 1) * BLOCK_LENGTH] for h in range(heads)], axis=1
        ).astype(BF16)
        return carry

    lax.fori_loop(0, blocks, one_block, 0)


def project_kernel(where_ref, att_ref, *refs, n_weights, kv_count, dp_count):
    w_refs = refs[:n_weights]
    mine_ref, other_ref, w_full = refs[n_weights:]
    tp = where_ref[2]
    half = mine_ref.shape[0]
    width = w_full.shape[2]
    place(w_refs, w_full, where_ref[0], where_ref[1], kv_count, dp_count)
    for out, which in ((other_ref, 1 - tp), (mine_ref, tp)):
        rows = att_ref[pl.ds(pl.multiple_of(which * half, half), half)]
        for k in range(w_full.shape[0]):
            out[:, k * width:(k + 1) * width] = jnp.dot(
                rows, w_full[k], preferred_element_type=F32
            ).astype(BF16)


def norm_kernel(a_ref, b_ref, gain_ref, out_ref):
    mixed = a_ref[...].astype(F32) + b_ref[...].astype(F32)
    scale = lax.rsqrt(jnp.mean(mixed * mixed, axis=-1, keepdims=True) + 1e-06)
    out_ref[...] = (mixed * scale * gain_ref[...]).astype(BF16)


def per_device(tokens, chosen, query_weight, key_matrix, value_matrix, out_weight, out_gain):
    kv_count = lax.axis_size("kv")
    dp_count = lax.axis_size("dp")
    tp_count = lax.axis_size("tp")
    kv = lax.axis_index("kv")
    dp = lax.axis_index("dp")
    tp = lax.axis_index("tp")
    where = jnp.stack([kv, dp, tp]).astype(jnp.int32)
    tok_rows, model = tokens.shape
    heads = query_weight.shape[1] // HEAD_WIDTH
    shard = query_weight.shape[0]
    direct = (
        dp_count == 4
        and kv_count <= 8
        and shard % (2 * dp_count * ALIGN) == 0
        and out_weight.shape[1] % 128 == 0
    )
    pair_shard = jnp.concatenate([key_matrix, value_matrix], axis=1)
    if direct:
        pair_parts = spread(pair_shard, kv_count, dp_count)
        q_parts = spread(query_weight, kv_count, dp_count)
        o_parts = spread(out_weight, kv_count, dp_count)
        pair_kernel = functools.partial(
            pair_project, n_weights=len(pair_parts), kv_count=kv_count, dp_count=dp_count
        )
    else:
        pair_parts = [lax.all_gather(pair_shard, "kv", axis=0, tiled=True)]
        q_parts = [lax.all_gather(query_weight, "kv", axis=0, tiled=True)]
        o_parts = [lax.all_gather(out_weight, "kv", axis=1, tiled=True)]
        pair_kernel = functools.partial(
            pair_project, n_weights=1, kv_count=kv_count, dp_count=dp_count
        )
    vmem = pl.BlockSpec(memory_space=pltpu.VMEM)
    smem = pl.BlockSpec(memory_space=pltpu.SMEM)
    pair_width = pair_shard.shape[1]
    pairs = pl.pallas_call(
        pair_kernel,
        out_shape=jax.ShapeDtypeStruct((tok_rows, pair_width), BF16),
        in_specs=[smem, vmem] + [vmem] * len(pair_parts),
        out_specs=vmem,
        scratch_shapes=[pltpu.VMEM((kv_count, shard, pair_width), BF16)]
        if direct
        else [pltpu.VMEM((1, model, pair_width), BF16)],
    )(where, tokens, *pair_parts)
    if direct:
        row_parts = [pairs] + [
            lax.ppermute(pairs, "kv", [(i, i + s) for i in range(kv_count - s)])
            for s in range(1, kv_count)
        ]
    else:
        row_parts = [lax.all_gather(pairs, "kv", axis=0, tiled=True)]
    attended = pl.pallas_call(
        functools.partial(
            attend_kernel,
            n_weights=len(q_parts),
            n_rows=len(row_parts),
            kv_count=kv_count,
            dp_count=dp_count,
            heads=heads,
        ),
        out_shape=jax.ShapeDtypeStruct((tok_rows, heads * HEAD_WIDTH), BF16),
        in_specs=[smem, smem, vmem] + [vmem] * (len(q_parts) + len(row_parts)),
        out_specs=vmem,
        scratch_shapes=[
            pltpu.VMEM((kv_count, shard, heads * HEAD_WIDTH) if direct else (1, model, heads * HEAD_WIDTH), BF16),
            pltpu.VMEM((kv_count * tok_rows, pair_width), BF16),
            pltpu.VMEM((tok_rows, heads * HEAD_WIDTH), BF16),
            pltpu.VMEM((chosen.shape[1] * BLOCK_LENGTH, pair_width), BF16),
        ],
    )(where, chosen, tokens, *q_parts, *row_parts)
    out_rows = tok_rows // tp_count
    head_rows, out_cols = out_weight.shape
    columns = out_cols * kv_count
    piece = jax.ShapeDtypeStruct((out_rows, columns), BF16)
    mine, other = pl.pallas_call(
        functools.partial(
            project_kernel, n_weights=len(o_parts), kv_count=kv_count, dp_count=dp_count
        ),
        out_shape=(piece, piece),
        in_specs=[smem, vmem] + [vmem] * len(o_parts),
        out_specs=(vmem, vmem),
        scratch_shapes=[
            pltpu.VMEM((kv_count, head_rows, out_cols) if direct else (1, head_rows, columns), BF16)
        ],
    )(where, attended, *o_parts)
    theirs = swap(other, "tp", 1, tp_count)
    return pl.pallas_call(
        norm_kernel,
        out_shape=jax.ShapeDtypeStruct((out_rows, columns), BF16),
        in_specs=[vmem, vmem, vmem],
        out_specs=vmem,
    )(mine, theirs, out_gain.reshape(1, -1))


def pair_project(where_ref, tok_ref, *refs, n_weights, kv_count, dp_count):
    w_refs = refs[:n_weights]
    out_ref, w_full = refs[n_weights:]
    place(w_refs, w_full, where_ref[0], where_ref[1], kv_count, dp_count)
    whole = w_full[...].reshape(-1, w_full.shape[-1])
    out_ref[...] = jnp.dot(tok_ref[...], whole, preferred_element_type=F32).astype(BF16)


def solution(mesh):
    placed = (
        P(("dp", "kv"), None),
        P(("dp", "kv"), None),
        P("kv", "tp"),
        P("kv", "tp"),
        P("kv", "tp"),
        P("tp", "kv"),
        P(),
    )
    return jax.shard_map(
        per_device,
        mesh=mesh,
        in_specs=placed,
        out_specs=P(("dp", "kv", "tp"), None),
        check_vma=False,
    )
```

```python
import functools

import jax
import jax.numpy as jnp
from jax import lax
from jax.experimental import pallas as pl
from jax.experimental.pallas import tpu as pltpu
from jax.sharding import PartitionSpec as P


HEAD_WIDTH = 64
BLOCK_LENGTH = 64
ALIGN = 16
LOG2E = 1.4426950408889634
BF16 = jnp.bfloat16
F32 = jnp.float32


def shift(x, axis, by, count):
    return lax.ppermute(x, axis, [(i, (i + by) % count) for i in range(count)])


def swap(x, axis, bit, count):
    return lax.ppermute(x, axis, [(i, i ^ bit) for i in range(count)])


def piece_of(w, dp_count):
    rows = w.shape[0] // dp_count
    return lax.dynamic_slice_in_dim(w, lax.axis_index("dp") * rows, rows, axis=0)


def along_kv(piece, kv_count):
    got = []
    for s in range(1, kv_count):
        got.append(shift(piece, "kv", s, kv_count))
    return got


def across_dp(w, got, dp_count):
    mine = jnp.concatenate(got, axis=0)
    parts = [w, mine]
    for bits in range(1, dp_count):
        parts.append(swap(mine, "dp", bits, dp_count))
    return parts


def place(refs, dest, kv, dp, kv_count):
    if len(refs) == 1:
        dest[...] = refs[0][...].reshape(dest.shape)
        return
    own = refs[0]
    dest[pl.ds(kv, 1)] = own[...][None]
    rows = own.shape[0] // (len(refs) - 1)
    for s in range(1, kv_count):
        source = lax.rem(kv - s + kv_count, kv_count)
        for bits, ref in enumerate(refs[1:]):
            first = pl.multiple_of((dp ^ bits) * rows, rows)
            dest[pl.ds(source, 1), pl.ds(first, rows)] = ref[(s - 1) * rows:s * rows][None]


def attend_kernel(where_ref, chosen_ref, tok_ref, *refs, n_weights, n_rows, kv_count, heads):
    w_refs = refs[:n_weights]
    row_refs = refs[n_weights:n_weights + n_rows]
    out_ref, w_full, kv_full, q_full, picked = refs[n_weights + n_rows:]
    kv = where_ref[0]
    dp = where_ref[1]
    place(w_refs, w_full, kv, dp, kv_count)
    if n_rows == 1:
        kv_full[...] = row_refs[0][...]
    else:
        count = row_refs[0].shape[0]
        for s, ref in enumerate(row_refs):
            source = lax.rem(kv - s + kv_count, kv_count)
            kv_full[pl.ds(pl.multiple_of(source * count, count), count)] = ref[...]
    whole = w_full[...].reshape(-1, w_full.shape[-1])
    queries = jnp.dot(tok_ref[...], whole, preferred_element_type=F32).astype(BF16)
    q_full[...] = queries
    blocks, sel = chosen_ref.shape
    wide = heads * BLOCK_LENGTH
    key_at = lax.broadcasted_iota(jnp.int32, (BLOCK_LENGTH, wide), 0)
    query_at = lax.rem(lax.broadcasted_iota(jnp.int32, (BLOCK_LENGTH, wide), 1), BLOCK_LENGTH)
    causal = key_at <= query_at
    factor = HEAD_WIDTH ** (-0.5) * LOG2E

    def one_block(g, carry):
        at = pl.multiple_of(g * BLOCK_LENGTH, BLOCK_LENGTH)
        qg = q_full[pl.ds(at, BLOCK_LENGTH)]
        stacked = jnp.concatenate(
            [qg[:, h * HEAD_WIDTH:(h + 1) * HEAD_WIDTH] for h in range(heads)], axis=0
        )
        stacked = jnp.concatenate([stacked, jnp.zeros_like(stacked)], axis=1)
        bias = []
        for s in range(sel):
            name = chosen_ref[g, s]
            first = pl.multiple_of(jnp.maximum(name, 0) * BLOCK_LENGTH, BLOCK_LENGTH)
            picked[s * BLOCK_LENGTH:(s + 1) * BLOCK_LENGTH] = kv_full[pl.ds(first, BLOCK_LENGTH)]
            bias.append(jnp.where(name < 0, F32(-1e30), F32(0)))
        pairs = picked[...]
        scores = lax.dot_general(
            pairs, stacked, (((1,), (1,)), ((), ())), preferred_element_type=F32
        )
        parts = []
        top = None
        for s in range(sel):
            part = scores[s * BLOCK_LENGTH:(s + 1) * BLOCK_LENGTH]
            part = jnp.where(causal, part, -1e30) if s == 0 else part + bias[s]
            parts.append(part)
            peak = jnp.max(part, axis=0, keepdims=True)
            top = peak if top is None else jnp.maximum(top, peak)
        total = None
        probs = []
        for part in parts:
            e = jnp.exp2((part - top) * factor)
            add = jnp.sum(e, axis=0, keepdims=True)
            total = add if total is None else total + add
            probs.append(e.astype(BF16))
        prob = jnp.concatenate(probs, axis=0)
        mixed = lax.dot_general(
            pairs, prob, (((0,), (0,)), ((), ())), preferred_element_type=F32
        )
        outcome = (mixed[HEAD_WIDTH:] / total).T
        out_ref[pl.ds(at, BLOCK_LENGTH)] = jnp.concatenate(
            [outcome[h * BLOCK_LENGTH:(h + 1) * BLOCK_LENGTH] for h in range(heads)], axis=1
        ).astype(BF16)
        return carry

    lax.fori_loop(0, blocks, one_block, 0)


def project_kernel(where_ref, att_ref, *refs, n_weights, kv_count):
    w_refs = refs[:n_weights]
    mine_ref, other_ref, w_full = refs[n_weights:]
    tp = where_ref[2]
    half = mine_ref.shape[0]
    width = w_full.shape[2]
    place(w_refs, w_full, where_ref[0], where_ref[1], kv_count)
    for out, which in ((other_ref, 1 - tp), (mine_ref, tp)):
        rows = att_ref[pl.ds(pl.multiple_of(which * half, half), half)]
        for k in range(w_full.shape[0]):
            out[:, k * width:(k + 1) * width] = jnp.dot(
                rows, w_full[k], preferred_element_type=F32
            ).astype(BF16)


def norm_kernel(a_ref, b_ref, gain_ref, out_ref):
    mixed = a_ref[...].astype(F32) + b_ref[...].astype(F32)
    scale = lax.rsqrt(jnp.mean(mixed * mixed, axis=-1, keepdims=True) + 1e-06)
    out_ref[...] = (mixed * scale * gain_ref[...]).astype(BF16)


def layer(tokens, chosen, query_weight, key_matrix, value_matrix, out_weight, out_gain):
    kv_count = lax.axis_size("kv")
    dp_count = lax.axis_size("dp")
    tp_count = lax.axis_size("tp")
    kv = lax.axis_index("kv")
    dp = lax.axis_index("dp")
    tp = lax.axis_index("tp")
    where = jnp.stack([kv, dp, tp]).astype(jnp.int32)
    tok_rows, model = tokens.shape
    heads = query_weight.shape[1] // HEAD_WIDTH
    shard = query_weight.shape[0]
    direct = (
        dp_count & (dp_count - 1) == 0
        and dp_count <= 8
        and kv_count <= 8
        and shard % (dp_count * ALIGN) == 0
        and out_weight.shape[1] % 128 == 0
    )
    if direct:
        pair_piece = jnp.concatenate(
            [piece_of(key_matrix, dp_count), piece_of(value_matrix, dp_count)], axis=1
        )
        pair_line = lax.all_gather(pair_piece, "kv", axis=0)
        q_piece, pair_line = lax.optimization_barrier((piece_of(query_weight, dp_count), pair_line))
        q_got = along_kv(q_piece, kv_count)
        pair_whole = lax.all_gather(pair_line, "dp", axis=0)
    else:
        pair_shard = jnp.concatenate([key_matrix, value_matrix], axis=1)
        pair_whole = lax.all_gather(pair_shard, "kv", axis=0)[None]
        q_parts = [lax.all_gather(query_weight, "kv", axis=0, tiled=True)]
        o_parts = [lax.all_gather(out_weight, "kv", axis=1, tiled=True)]
    vmem = pl.BlockSpec(memory_space=pltpu.VMEM)
    smem = pl.BlockSpec(memory_space=pltpu.SMEM)
    pair_width = pair_whole.shape[-1]
    pairs = pl.pallas_call(
        pair_project,
        out_shape=jax.ShapeDtypeStruct((tok_rows, pair_width), BF16),
        in_specs=[vmem, vmem],
        out_specs=vmem,
        scratch_shapes=[pltpu.VMEM((model, pair_width), BF16)],
    )(tokens, pair_whole)
    if direct:
        row_parts = [pairs]
        for s in range(1, kv_count):
            row_parts.append(lax.ppermute(pairs, "kv", [(i, i + s) for i in range(kv_count - s)]))
        q_parts = across_dp(query_weight, q_got, dp_count)
        o_got = along_kv(piece_of(out_weight, dp_count), kv_count)
        o_parts = across_dp(out_weight, o_got, dp_count)
    else:
        row_parts = [lax.all_gather(pairs, "kv", axis=0, tiled=True)]
    attended = pl.pallas_call(
        functools.partial(
            attend_kernel,
            n_weights=len(q_parts),
            n_rows=len(row_parts),
            kv_count=kv_count,
            heads=heads,
        ),
        out_shape=jax.ShapeDtypeStruct((tok_rows, heads * HEAD_WIDTH), BF16),
        in_specs=[smem, smem, vmem] + [vmem] * (len(q_parts) + len(row_parts)),
        out_specs=vmem,
        scratch_shapes=[
            pltpu.VMEM((kv_count, shard, heads * HEAD_WIDTH) if direct else (1, model, heads * HEAD_WIDTH), BF16),
            pltpu.VMEM((kv_count * tok_rows, pair_width), BF16),
            pltpu.VMEM((tok_rows, heads * HEAD_WIDTH), BF16),
            pltpu.VMEM((chosen.shape[1] * BLOCK_LENGTH, pair_width), BF16),
        ],
        cost_estimate=pl.CostEstimate(
            flops=64 * tok_rows * model * heads * HEAD_WIDTH,
            bytes_accessed=2 * tok_rows * model,
            transcendentals=0,
        ),
    )(where, chosen, tokens, *q_parts, *row_parts)
    out_rows = tok_rows // tp_count
    head_rows, out_cols = out_weight.shape
    columns = out_cols * kv_count
    piece = jax.ShapeDtypeStruct((out_rows, columns), BF16)
    mine, other = pl.pallas_call(
        functools.partial(
            project_kernel, n_weights=len(o_parts), kv_count=kv_count
        ),
        out_shape=(piece, piece),
        in_specs=[smem, vmem] + [vmem] * len(o_parts),
        out_specs=(vmem, vmem),
        scratch_shapes=[
            pltpu.VMEM((kv_count, head_rows, out_cols) if direct else (1, head_rows, columns), BF16)
        ],
    )(where, attended, *o_parts)
    theirs = swap(other, "tp", 1, tp_count)
    return pl.pallas_call(
        norm_kernel,
        out_shape=jax.ShapeDtypeStruct((out_rows, columns), BF16),
        in_specs=[vmem, vmem, vmem],
        out_specs=vmem,
    )(mine, theirs, out_gain.reshape(1, -1))


def pair_project(tok_ref, w_ref, out_ref, w_full):
    dp_count, kv_count, rows = w_ref.shape[:3]
    for k in range(kv_count):
        for d in range(dp_count):
            at = (k * dp_count + d) * rows
            w_full[at:at + rows] = w_ref[d, k]
    out_ref[...] = jnp.dot(tok_ref[...], w_full[...], preferred_element_type=F32).astype(BF16)


def solution(mesh):
    placed = (
        P(("dp", "kv"), None),
        P(("dp", "kv"), None),
        P("kv", "tp"),
        P("kv", "tp"),
        P("kv", "tp"),
        P("tp", "kv"),
        P(),
    )
    return jax.shard_map(
        layer,
        mesh=mesh,
        in_specs=placed,
        out_specs=P(("dp", "kv", "tp"), None),
        check_vma=False,
    )
```

```python
import functools

import jax
import jax.numpy as jnp
from jax import lax
from jax.experimental import pallas as pl
from jax.experimental.pallas import tpu as pltpu
from jax.sharding import PartitionSpec as P


HEAD_WIDTH = 64
BLOCK_LENGTH = 64
ALIGN = 16
LOG2E = 1.4426950408889634
BF16 = jnp.bfloat16
F32 = jnp.float32


def shift(x, axis, by, count):
    return lax.ppermute(x, axis, [(i, (i + by) % count) for i in range(count)])


def swap(x, axis, bit, count):
    return lax.ppermute(x, axis, [(i, i ^ bit) for i in range(count)])


def piece_of(w, dp_count):
    rows = w.shape[0] // dp_count
    return lax.dynamic_slice_in_dim(w, lax.axis_index("dp") * rows, rows, axis=0)


def along_kv(piece, kv_count):
    got = []
    for s in range(1, kv_count):
        got.append(shift(piece, "kv", s, kv_count))
    return got


def across_dp(w, got, dp_count):
    mine = jnp.concatenate(got, axis=0)
    parts = [w, mine]
    for bits in range(1, dp_count):
        parts.append(swap(mine, "dp", bits, dp_count))
    return parts


def place(refs, dest, kv, dp, kv_count):
    if len(refs) == 1:
        dest[...] = refs[0][...].reshape(dest.shape)
        return
    own = refs[0]
    dest[pl.ds(kv, 1)] = own[...][None]
    rows = own.shape[0] // (len(refs) - 1)
    for s in range(1, kv_count):
        source = lax.rem(kv - s + kv_count, kv_count)
        for bits, ref in enumerate(refs[1:]):
            first = pl.multiple_of((dp ^ bits) * rows, rows)
            dest[pl.ds(source, 1), pl.ds(first, rows)] = ref[(s - 1) * rows:s * rows][None]


def attend_kernel(where_ref, chosen_ref, tok_ref, *refs, n_weights, n_rows, kv_count, heads):
    w_refs = refs[:n_weights]
    row_refs = refs[n_weights:n_weights + n_rows]
    out_ref, w_full, kv_full, q_full, picked = refs[n_weights + n_rows:]
    kv = where_ref[0]
    dp = where_ref[1]
    place(w_refs, w_full, kv, dp, kv_count)
    if n_rows == 1:
        kv_full[...] = row_refs[0][...]
    else:
        count = row_refs[0].shape[0]
        for s, ref in enumerate(row_refs):
            source = lax.rem(kv - s + kv_count, kv_count)
            kv_full[pl.ds(pl.multiple_of(source * count, count), count)] = ref[...]
    whole = w_full[...].reshape(-1, w_full.shape[-1])
    queries = jnp.dot(tok_ref[...], whole, preferred_element_type=F32).astype(BF16)
    q_full[...] = queries
    blocks, sel = chosen_ref.shape
    wide = heads * BLOCK_LENGTH
    key_at = lax.broadcasted_iota(jnp.int32, (BLOCK_LENGTH, wide), 0)
    query_at = lax.rem(lax.broadcasted_iota(jnp.int32, (BLOCK_LENGTH, wide), 1), BLOCK_LENGTH)
    causal = key_at <= query_at
    factor = HEAD_WIDTH ** (-0.5) * LOG2E

    def one_block(g, carry):
        at = pl.multiple_of(g * BLOCK_LENGTH, BLOCK_LENGTH)
        qg = q_full[pl.ds(at, BLOCK_LENGTH)]
        stacked = jnp.concatenate(
            [qg[:, h * HEAD_WIDTH:(h + 1) * HEAD_WIDTH] for h in range(heads)], axis=0
        )
        stacked = jnp.concatenate([stacked, jnp.zeros_like(stacked)], axis=1)
        bias = []
        for s in range(sel):
            name = chosen_ref[g, s]
            first = pl.multiple_of(jnp.maximum(name, 0) * BLOCK_LENGTH, BLOCK_LENGTH)
            picked[s * BLOCK_LENGTH:(s + 1) * BLOCK_LENGTH] = kv_full[pl.ds(first, BLOCK_LENGTH)]
            bias.append(jnp.where(name < 0, F32(-1e30), F32(0)))
        pairs = picked[...]
        scores = lax.dot_general(
            pairs, stacked, (((1,), (1,)), ((), ())), preferred_element_type=F32
        )
        parts = []
        top = None
        for s in range(sel):
            part = scores[s * BLOCK_LENGTH:(s + 1) * BLOCK_LENGTH]
            part = jnp.where(causal, part, -1e30) if s == 0 else part + bias[s]
            parts.append(part)
            peak = jnp.max(part, axis=0, keepdims=True)
            top = peak if top is None else jnp.maximum(top, peak)
        total = None
        probs = []
        for part in parts:
            e = jnp.exp2((part - top) * factor)
            add = jnp.sum(e, axis=0, keepdims=True)
            total = add if total is None else total + add
            probs.append(e.astype(BF16))
        prob = jnp.concatenate(probs, axis=0)
        mixed = lax.dot_general(
            pairs, prob, (((0,), (0,)), ((), ())), preferred_element_type=F32
        )
        outcome = (mixed[HEAD_WIDTH:] / total).T
        out_ref[pl.ds(at, BLOCK_LENGTH)] = jnp.concatenate(
            [outcome[h * BLOCK_LENGTH:(h + 1) * BLOCK_LENGTH] for h in range(heads)], axis=1
        ).astype(BF16)
        return carry

    lax.fori_loop(0, blocks, one_block, 0, unroll=2)


def project_kernel(where_ref, att_ref, *refs, n_weights, kv_count):
    w_refs = refs[:n_weights]
    mine_ref, other_ref, w_full = refs[n_weights:]
    tp = where_ref[2]
    half = mine_ref.shape[0]
    width = w_full.shape[2]
    place(w_refs, w_full, where_ref[0], where_ref[1], kv_count)
    for out, which in ((other_ref, 1 - tp), (mine_ref, tp)):
        rows = att_ref[pl.ds(pl.multiple_of(which * half, half), half)]
        for k in range(w_full.shape[0]):
            out[:, k * width:(k + 1) * width] = jnp.dot(
                rows, w_full[k], preferred_element_type=F32
            ).astype(BF16)


def norm_kernel(a_ref, b_ref, gain_ref, out_ref):
    mixed = a_ref[...].astype(F32) + b_ref[...].astype(F32)
    scale = lax.rsqrt(jnp.mean(mixed * mixed, axis=-1, keepdims=True) + 1e-06)
    out_ref[...] = (mixed * scale * gain_ref[...]).astype(BF16)


def layer(tokens, chosen, query_weight, key_matrix, value_matrix, out_weight, out_gain):
    kv_count = lax.axis_size("kv")
    dp_count = lax.axis_size("dp")
    tp_count = lax.axis_size("tp")
    kv = lax.axis_index("kv")
    dp = lax.axis_index("dp")
    tp = lax.axis_index("tp")
    where = jnp.stack([kv, dp, tp]).astype(jnp.int32)
    tok_rows, model = tokens.shape
    heads = query_weight.shape[1] // HEAD_WIDTH
    shard = query_weight.shape[0]
    direct = (
        dp_count & (dp_count - 1) == 0
        and dp_count <= 8
        and kv_count <= 8
        and shard % (dp_count * ALIGN) == 0
        and out_weight.shape[1] % 128 == 0
    )
    if direct:
        columns = query_weight.shape[1]
        both = jnp.concatenate(
            [
                piece_of(query_weight, dp_count),
                piece_of(key_matrix, dp_count),
                piece_of(value_matrix, dp_count),
            ],
            axis=1,
        )
        got = along_kv(both, kv_count)
        pair_shard = jnp.concatenate([key_matrix, value_matrix], axis=1)
        pair_parts = across_dp(pair_shard, [g[:, columns:] for g in got], dp_count)
        q_parts = across_dp(query_weight, [g[:, :columns] for g in got], dp_count)
        o_got = along_kv(piece_of(out_weight, dp_count), kv_count)
        o_parts = across_dp(out_weight, o_got, dp_count)
    else:
        pair_shard = jnp.concatenate([key_matrix, value_matrix], axis=1)
        pair_parts = [lax.all_gather(pair_shard, "kv", axis=0, tiled=True)]
        q_parts = [lax.all_gather(query_weight, "kv", axis=0, tiled=True)]
        o_parts = [lax.all_gather(out_weight, "kv", axis=1, tiled=True)]
    vmem = pl.BlockSpec(memory_space=pltpu.VMEM)
    smem = pl.BlockSpec(memory_space=pltpu.SMEM)
    pair_width = pair_shard.shape[1]
    pairs = pl.pallas_call(
        functools.partial(pair_project, kv_count=kv_count),
        out_shape=jax.ShapeDtypeStruct((tok_rows, pair_width), BF16),
        in_specs=[smem, vmem] + [vmem] * len(pair_parts),
        out_specs=vmem,
        scratch_shapes=[
            pltpu.VMEM((kv_count, shard, pair_width) if direct else (1, model, pair_width), BF16)
        ],
    )(where, tokens, *pair_parts)
    if direct:
        row_parts = [pairs]
        for s in range(1, kv_count):
            row_parts.append(lax.ppermute(pairs, "kv", [(i, i + s) for i in range(kv_count - s)]))
    else:
        row_parts = [lax.all_gather(pairs, "kv", axis=0, tiled=True)]
    attended = pl.pallas_call(
        functools.partial(
            attend_kernel,
            n_weights=len(q_parts),
            n_rows=len(row_parts),
            kv_count=kv_count,
            heads=heads,
        ),
        out_shape=jax.ShapeDtypeStruct((tok_rows, heads * HEAD_WIDTH), BF16),
        in_specs=[smem, smem, vmem] + [vmem] * (len(q_parts) + len(row_parts)),
        out_specs=vmem,
        scratch_shapes=[
            pltpu.VMEM((kv_count, shard, heads * HEAD_WIDTH) if direct else (1, model, heads * HEAD_WIDTH), BF16),
            pltpu.VMEM((kv_count * tok_rows, pair_width), BF16),
            pltpu.VMEM((tok_rows, heads * HEAD_WIDTH), BF16),
            pltpu.VMEM((chosen.shape[1] * BLOCK_LENGTH, pair_width), BF16),
        ],
        cost_estimate=pl.CostEstimate(
            flops=64 * tok_rows * model * heads * HEAD_WIDTH,
            bytes_accessed=2 * tok_rows * model,
            transcendentals=0,
        ),
    )(where, chosen, tokens, *q_parts, *row_parts)
    out_rows = tok_rows // tp_count
    head_rows, out_cols = out_weight.shape
    columns = out_cols * kv_count
    piece = jax.ShapeDtypeStruct((out_rows, columns), BF16)
    mine, other = pl.pallas_call(
        functools.partial(
            project_kernel, n_weights=len(o_parts), kv_count=kv_count
        ),
        out_shape=(piece, piece),
        in_specs=[smem, vmem] + [vmem] * len(o_parts),
        out_specs=(vmem, vmem),
        scratch_shapes=[
            pltpu.VMEM((kv_count, head_rows, out_cols) if direct else (1, head_rows, columns), BF16)
        ],
    )(where, attended, *o_parts)
    theirs = swap(other, "tp", 1, tp_count)
    return pl.pallas_call(
        norm_kernel,
        out_shape=jax.ShapeDtypeStruct((out_rows, columns), BF16),
        in_specs=[vmem, vmem, vmem],
        out_specs=vmem,
    )(mine, theirs, out_gain.reshape(1, -1))


def pair_project(where_ref, tok_ref, *refs, kv_count):
    *w_refs, out_ref, w_full = refs
    place(w_refs, w_full, where_ref[0], where_ref[1], kv_count)
    whole = w_full[...].reshape(-1, w_full.shape[-1])
    out_ref[...] = jnp.dot(tok_ref[...], whole, preferred_element_type=F32).astype(BF16)


def solution(mesh):
    placed = (
        P(("dp", "kv"), None),
        P(("dp", "kv"), None),
        P("kv", "tp"),
        P("kv", "tp"),
        P("kv", "tp"),
        P("tp", "kv"),
        P(),
    )
    return jax.shard_map(
        layer,
        mesh=mesh,
        in_specs=placed,
        out_specs=P(("dp", "kv", "tp"), None),
        check_vma=False,
    )
```

```python
import functools

import jax
import jax.numpy as jnp
from jax import lax
from jax.experimental import pallas as pl
from jax.experimental.pallas import tpu as pltpu
from jax.sharding import PartitionSpec as P


HEAD_WIDTH = 64
BLOCK_LENGTH = 64
ALIGN = 16
LOG2E = 1.4426950408889634
BF16 = jnp.bfloat16
F32 = jnp.float32


def shift(x, axis, by, count):
    return lax.ppermute(x, axis, [(i, (i + by) % count) for i in range(count)])


def swap(x, axis, bit, count):
    return lax.ppermute(x, axis, [(i, i ^ bit) for i in range(count)])


def piece_of(w, dp_count):
    rows = w.shape[0] // dp_count
    return lax.dynamic_slice_in_dim(w, lax.axis_index("dp") * rows, rows, axis=0)


def along_kv(piece, kv_count):
    got = []
    for s in range(1, kv_count):
        got.append(shift(piece, "kv", s, kv_count))
    return got


def across_dp(w, got, dp_count):
    mine = jnp.concatenate(got, axis=0)
    parts = [w, mine]
    for bits in range(1, dp_count):
        parts.append(swap(mine, "dp", bits, dp_count))
    return parts


def place(refs, dest, kv, dp, kv_count):
    if len(refs) == 1:
        dest[...] = refs[0][...].reshape(dest.shape)
        return
    own = refs[0]
    dest[pl.ds(kv, 1)] = own[...][None]
    rows = own.shape[0] // (len(refs) - 1)
    for s in range(1, kv_count):
        source = lax.rem(kv - s + kv_count, kv_count)
        for bits, ref in enumerate(refs[1:]):
            first = pl.multiple_of((dp ^ bits) * rows, rows)
            dest[pl.ds(source, 1), pl.ds(first, rows)] = ref[(s - 1) * rows:s * rows][None]


def attend_kernel(where_ref, chosen_ref, tok_ref, *refs, n_weights, n_rows, kv_count, heads):
    w_refs = refs[:n_weights]
    row_refs = refs[n_weights:n_weights + n_rows]
    out_ref, w_full, kv_full, q_full, picked = refs[n_weights + n_rows:]
    kv = where_ref[0]
    dp = where_ref[1]
    place(w_refs, w_full, kv, dp, kv_count)
    if n_rows == 1:
        kv_full[...] = row_refs[0][...]
    else:
        count = row_refs[0].shape[0]
        for s, ref in enumerate(row_refs):
            source = lax.rem(kv - s + kv_count, kv_count)
            kv_full[pl.ds(pl.multiple_of(source * count, count), count)] = ref[...]
    whole = w_full[...].reshape(-1, w_full.shape[-1])
    queries = jnp.dot(tok_ref[...], whole, preferred_element_type=F32).astype(BF16)
    q_full[...] = queries
    blocks, sel = chosen_ref.shape
    wide = heads * BLOCK_LENGTH
    key_at = lax.broadcasted_iota(jnp.int32, (BLOCK_LENGTH, wide), 0)
    query_at = lax.rem(lax.broadcasted_iota(jnp.int32, (BLOCK_LENGTH, wide), 1), BLOCK_LENGTH)
    causal = key_at <= query_at
    factor = HEAD_WIDTH ** (-0.5) * LOG2E

    def one_block(g, carry):
        at = pl.multiple_of(g * BLOCK_LENGTH, BLOCK_LENGTH)
        qg = q_full[pl.ds(at, BLOCK_LENGTH)]
        stacked = jnp.concatenate(
            [qg[:, h * HEAD_WIDTH:(h + 1) * HEAD_WIDTH] for h in range(heads)], axis=0
        )
        stacked = jnp.concatenate([stacked, jnp.zeros_like(stacked)], axis=1)
        bias = []
        for s in range(sel):
            name = chosen_ref[g, s]
            first = pl.multiple_of(jnp.maximum(name, 0) * BLOCK_LENGTH, BLOCK_LENGTH)
            picked[s * BLOCK_LENGTH:(s + 1) * BLOCK_LENGTH] = kv_full[pl.ds(first, BLOCK_LENGTH)]
            bias.append(jnp.where(name < 0, F32(-1e30), F32(0)))
        pairs = picked[...]
        scores = lax.dot_general(
            pairs, stacked, (((1,), (1,)), ((), ())), preferred_element_type=F32
        )
        parts = []
        top = None
        for s in range(sel):
            part = scores[s * BLOCK_LENGTH:(s + 1) * BLOCK_LENGTH]
            part = jnp.where(causal, part, -1e30) if s == 0 else part + bias[s]
            parts.append(part)
            peak = jnp.max(part, axis=0, keepdims=True)
            top = peak if top is None else jnp.maximum(top, peak)
        total = None
        probs = []
        for part in parts:
            e = jnp.exp2((part - top) * factor)
            add = jnp.sum(e, axis=0, keepdims=True)
            total = add if total is None else total + add
            probs.append(e.astype(BF16))
        prob = jnp.concatenate(probs, axis=0)
        mixed = lax.dot_general(
            pairs, prob, (((0,), (0,)), ((), ())), preferred_element_type=F32
        )
        outcome = (mixed[HEAD_WIDTH:] / total).T
        out_ref[pl.ds(at, BLOCK_LENGTH)] = jnp.concatenate(
            [outcome[h * BLOCK_LENGTH:(h + 1) * BLOCK_LENGTH] for h in range(heads)], axis=1
        ).astype(BF16)
        return carry

    lax.fori_loop(0, blocks, one_block, 0, unroll=4)


def project_kernel(where_ref, att_ref, *refs, n_weights, kv_count):
    w_refs = refs[:n_weights]
    mine_ref, other_ref, w_full = refs[n_weights:]
    tp = where_ref[2]
    half = mine_ref.shape[0]
    width = w_full.shape[2]
    place(w_refs, w_full, where_ref[0], where_ref[1], kv_count)
    for out, which in ((other_ref, 1 - tp), (mine_ref, tp)):
        rows = att_ref[pl.ds(pl.multiple_of(which * half, half), half)]
        for k in range(w_full.shape[0]):
            out[:, k * width:(k + 1) * width] = jnp.dot(
                rows, w_full[k], preferred_element_type=F32
            ).astype(BF16)


def norm_kernel(a_ref, b_ref, gain_ref, out_ref):
    mixed = a_ref[...].astype(F32) + b_ref[...].astype(F32)
    scale = lax.rsqrt(jnp.mean(mixed * mixed, axis=-1, keepdims=True) + 1e-06)
    out_ref[...] = (mixed * scale * gain_ref[...]).astype(BF16)


def layer(tokens, chosen, query_weight, key_matrix, value_matrix, out_weight, out_gain):
    kv_count = lax.axis_size("kv")
    dp_count = lax.axis_size("dp")
    tp_count = lax.axis_size("tp")
    kv = lax.axis_index("kv")
    dp = lax.axis_index("dp")
    tp = lax.axis_index("tp")
    where = jnp.stack([kv, dp, tp]).astype(jnp.int32)
    tok_rows, model = tokens.shape
    heads = query_weight.shape[1] // HEAD_WIDTH
    shard = query_weight.shape[0]
    direct = (
        dp_count & (dp_count - 1) == 0
        and dp_count <= 8
        and kv_count <= 8
        and shard % (dp_count * ALIGN) == 0
        and out_weight.shape[1] % 128 == 0
    )
    if direct:
        columns = query_weight.shape[1]
        both = jnp.concatenate(
            [
                piece_of(query_weight, dp_count),
                piece_of(key_matrix, dp_count),
                piece_of(value_matrix, dp_count),
            ],
            axis=1,
        )
        got = along_kv(both, kv_count)
        late_key, late_value, *got = lax.optimization_barrier((key_matrix, value_matrix, *got))
        pair_shard = jnp.concatenate([late_key, late_value], axis=1)
        pair_parts = across_dp(pair_shard, [g[:, columns:] for g in got], dp_count)
        q_parts = across_dp(query_weight, [g[:, :columns] for g in got], dp_count)
        o_got = along_kv(piece_of(out_weight, dp_count), kv_count)
        o_parts = across_dp(out_weight, o_got, dp_count)
    else:
        pair_shard = jnp.concatenate([key_matrix, value_matrix], axis=1)
        pair_parts = [lax.all_gather(pair_shard, "kv", axis=0, tiled=True)]
        q_parts = [lax.all_gather(query_weight, "kv", axis=0, tiled=True)]
        o_parts = [lax.all_gather(out_weight, "kv", axis=1, tiled=True)]
    vmem = pl.BlockSpec(memory_space=pltpu.VMEM)
    smem = pl.BlockSpec(memory_space=pltpu.SMEM)
    pair_width = pair_shard.shape[1]
    pairs = pl.pallas_call(
        functools.partial(pair_project, kv_count=kv_count),
        out_shape=jax.ShapeDtypeStruct((tok_rows, pair_width), BF16),
        in_specs=[smem, vmem] + [vmem] * len(pair_parts),
        out_specs=vmem,
        scratch_shapes=[
            pltpu.VMEM((kv_count, shard, pair_width) if direct else (1, model, pair_width), BF16)
        ],
    )(where, tokens, *pair_parts)
    if direct:
        row_parts = [pairs]
        for s in range(1, kv_count):
            row_parts.append(lax.ppermute(pairs, "kv", [(i, i + s) for i in range(kv_count - s)]))
    else:
        row_parts = [lax.all_gather(pairs, "kv", axis=0, tiled=True)]
    attended = pl.pallas_call(
        functools.partial(
            attend_kernel,
            n_weights=len(q_parts),
            n_rows=len(row_parts),
            kv_count=kv_count,
            heads=heads,
        ),
        out_shape=jax.ShapeDtypeStruct((tok_rows, heads * HEAD_WIDTH), BF16),
        in_specs=[smem, smem, vmem] + [vmem] * (len(q_parts) + len(row_parts)),
        out_specs=vmem,
        scratch_shapes=[
            pltpu.VMEM((kv_count, shard, heads * HEAD_WIDTH) if direct else (1, model, heads * HEAD_WIDTH), BF16),
            pltpu.VMEM((kv_count * tok_rows, pair_width), BF16),
            pltpu.VMEM((tok_rows, heads * HEAD_WIDTH), BF16),
            pltpu.VMEM((chosen.shape[1] * BLOCK_LENGTH, pair_width), BF16),
        ],
        cost_estimate=pl.CostEstimate(
            flops=64 * tok_rows * model * heads * HEAD_WIDTH,
            bytes_accessed=2 * tok_rows * model,
            transcendentals=0,
        ),
    )(where, chosen, tokens, *q_parts, *row_parts)
    out_rows = tok_rows // tp_count
    head_rows, out_cols = out_weight.shape
    columns = out_cols * kv_count
    piece = jax.ShapeDtypeStruct((out_rows, columns), BF16)
    mine, other = pl.pallas_call(
        functools.partial(
            project_kernel, n_weights=len(o_parts), kv_count=kv_count
        ),
        out_shape=(piece, piece),
        in_specs=[smem, vmem] + [vmem] * len(o_parts),
        out_specs=(vmem, vmem),
        scratch_shapes=[
            pltpu.VMEM((kv_count, head_rows, out_cols) if direct else (1, head_rows, columns), BF16)
        ],
    )(where, attended, *o_parts)
    theirs = swap(other, "tp", 1, tp_count)
    steps = 4 if out_rows % (4 * ALIGN) == 0 else 1
    tall = pl.BlockSpec((out_rows // steps, columns), lambda i: (i, 0))
    return pl.pallas_call(
        norm_kernel,
        grid=(steps,),
        out_shape=jax.ShapeDtypeStruct((out_rows, columns), BF16),
        in_specs=[tall, tall, pl.BlockSpec((1, columns), lambda i: (0, 0))],
        out_specs=tall,
    )(mine, theirs, out_gain.reshape(1, -1))


def pair_project(where_ref, tok_ref, *refs, kv_count):
    *w_refs, out_ref, w_full = refs
    place(w_refs, w_full, where_ref[0], where_ref[1], kv_count)
    whole = w_full[...].reshape(-1, w_full.shape[-1])
    out_ref[...] = jnp.dot(tok_ref[...], whole, preferred_element_type=F32).astype(BF16)


def solution(mesh):
    placed = (
        P(("dp", "kv"), None),
        P(("dp", "kv"), None),
        P("kv", "tp"),
        P("kv", "tp"),
        P("kv", "tp"),
        P("tp", "kv"),
        P(),
    )
    return jax.shard_map(
        layer,
        mesh=mesh,
        in_specs=placed,
        out_specs=P(("dp", "kv", "tp"), None),
        check_vma=False,
    )
```
